32 devices in a mesh: sp: 8 (over z, y), tp: 4 (over x, core).
Axes of the slice: x: 2, y: 2, z: 4, core: 2. Of those that a mesh axis runs over, the one named last changes fastest.
Arguments:
- inputs: bfloat16 [2, 3072, 4096], P(None, 'sp'), may hold values from -8 to 8
- w_key: bfloat16 [4096, 2048], P(None, 'tp'), may hold values from -0.09375 to 0.09375
- w_value: bfloat16 [4096, 2048], P(None, 'tp'), may hold values from -0.09375 to 0.09375
- w_query: bfloat16 [4096, 2048], P(None, 'tp'), may hold values from -0.09375 to 0.09375
- w_igate: bfloat16 [4096, 16], replicated, may hold values from -1 to 1
- w_fgate: bfloat16 [4096, 16], replicated, may hold values from -0.09375 to 0.09375
- forget_bias: float32 [16], replicated, may hold values from 3 to 12
- new_rows: bfloat16 [2, 4096], P(None, 'tp'), may hold values from -6 to 6
Outputs:
- cache_matrix: bfloat16 [2, 16, 128, 128], P(None, 'tp', 'sp')
- cache_normal: float32 [2, 16, 128], P(None, 'tp', 'sp')
- cache_top: float32 [2, 16], P(None, 'tp')
- read: bfloat16 [2, 16, 128], P(None, 'tp', 'sp')
The draws below stay inside these ranges and needn't reach their ends.
All inputs are finite; a program needn't handle non-finite values.
Results may differ from the reference program's by a relative error of at most 0.015.
Values may be sent and summed in bfloat16 or wider, within the bound.
A program may use at most 64 MiB of HBM per device.

```python
import jax
import jax.numpy as jnp
from jax import lax

D = 4096
H = 16
DH = 128
SEQS = 2
LEN = 3072


def draw_inputs(key, part):
    noise_key, shift_key, pick_key, chosen_key = jax.random.split(jax.random.fold_in(key, 3), 4)
    drawn = jax.random.normal(noise_key, (SEQS, LEN, D), jnp.float32)
    shifts = 1.5 * jax.random.normal(shift_key, (SEQS, LEN // 32, 1, D), jnp.float32)
    drawn = drawn + jnp.broadcast_to(shifts, (SEQS, LEN // 32, 32, D)).reshape(SEQS, LEN, D)
    return jnp.clip(drawn, -8.0, 8.0).astype(jnp.bfloat16)


def draw_w_igate(key, part):
    drawn = jax.random.normal(jax.random.fold_in(key, 5), (D, H), jnp.float32) / jnp.sqrt(D * 1.0)
    return jnp.clip(drawn, -1.0, 1.0).astype(jnp.bfloat16)


def draw_forget_bias(key, part):
    pick_key, jitter_key = jax.random.split(jax.random.fold_in(key, 9))
    slow_share = 0.5
    is_slow = jax.random.uniform(pick_key, (H,), jnp.float32) < slow_share
    jitter = jax.random.uniform(jitter_key, (H,), jnp.float32, -0.3, 0.3)
    return jnp.where(is_slow, jnp.log(LEN * 1.0) + 1.0, 3.5) + jitter


def steps_of(rng, dims, cuts, low, top_value):
    level, own = 1.0, jax.random.fold_in(rng, 6)
    for axis_at, blocks in cuts:
        steps = jnp.exp(jax.random.uniform(jax.random.fold_in(own, axis_at), (blocks,), jnp.float32, low / len(cuts), top_value / len(cuts)))
        level = level * jnp.repeat(steps, dims[axis_at] // blocks).reshape([-1 if axis == axis_at else 1 for axis in range(len(dims))])
    return level


def scatter_about(own_key, dims, spread, limit, cuts=(), kind=jnp.bfloat16):
    loudness = steps_of(own_key, dims, cuts, -0.22, 0.18) if cuts else 1.0
    values = jax.random.normal(own_key, dims, jnp.float32) * spread * loudness
    return jnp.minimum(jnp.maximum(values, -limit), limit).astype(kind)


def setup_inputs(seed: int = 0) -> dict:
    seeds = jax.random.split(jax.random.key(seed), 9)
    return {
        "inputs": draw_inputs(jax.random.fold_in(seeds[8], 71), 0),
        "w_key": scatter_about(seeds[1], (D, H * DH), D ** -0.5, 0.09375, ((1, 4),)),
        "w_value": scatter_about(seeds[2], (D, H * DH), D ** -0.5, 0.09375, ((1, 4),)),
        "w_query": scatter_about(seeds[3], (D, H * DH), D ** -0.5, 0.09375, ((1, 4),)),
        "w_igate": draw_w_igate(jax.random.fold_in(seeds[8], 71), 0),
        "w_fgate": scatter_about(seeds[5], (D, H), D ** -0.5, 0.09375),
        "forget_bias": draw_forget_bias(jax.random.fold_in(seeds[8], 71), 0),
        "new_rows": scatter_about(seeds[7], (SEQS, D), 1.0, 6.0, ((1, 4),)),
    }


EPS = 1e-06

def normalize(row_block):
    scaled = row_block.astype(jnp.float32)
    scaled = scaled * lax.rsqrt(lax.optimization_barrier(jnp.mean(scaled * scaled, axis=-1, keepdims=True)) + EPS)
    return scaled.astype(jnp.bfloat16)

def reference(inputs, w_key, w_value, w_query, w_igate, w_fgate, forget_bias, new_rows):

    def per_sequence(row_block):
        normed = normalize(row_block)
        key_heads = jnp.dot(normed, w_key, preferred_element_type=jnp.float32).astype(jnp.bfloat16).reshape(LEN, H, DH)
        value_heads = jnp.dot(normed, w_value, preferred_element_type=jnp.float32).astype(jnp.bfloat16).reshape(LEN, H, DH)
        input_pre = jnp.dot(normed, w_igate, preferred_element_type=jnp.float32)
        log_forget = jax.nn.log_sigmoid(jnp.dot(normed, w_fgate, preferred_element_type=jnp.float32) + forget_bias)
        running = jnp.cumsum(log_forget, axis=0)
        log_weight = running[-1:, :] - running + input_pre
        stabilizer = lax.optimization_barrier(jnp.max(log_weight, axis=0))
        weight = jnp.exp(log_weight - stabilizer[None, :])
        weighted = (weight[:, :, None] * value_heads.astype(jnp.float32)).astype(jnp.bfloat16)
        matrix = jnp.einsum('the,thd->hed', weighted.astype(jnp.float32), key_heads.astype(jnp.float32))
        normal = jnp.einsum('th,thd->hd', weight, key_heads.astype(jnp.float32))
        return (matrix.astype(jnp.bfloat16), normal, stabilizer)
    cache_matrix, cache_normal, cache_top = lax.map(per_sequence, inputs)
    seq_count = new_rows.shape[0]
    new_normed = normalize(new_rows)
    query_new = jnp.dot(new_normed, w_query, preferred_element_type=jnp.float32).astype(jnp.bfloat16)
    key_new = jnp.dot(new_normed, w_key, preferred_element_type=jnp.float32).astype(jnp.bfloat16)
    value_new = jnp.dot(new_normed, w_value, preferred_element_type=jnp.float32).astype(jnp.bfloat16)
    query_new = query_new.astype(jnp.float32).reshape(seq_count, H, DH)
    key_new = key_new.astype(jnp.float32).reshape(seq_count, H, DH)
    value_new = value_new.astype(jnp.float32).reshape(seq_count, H, DH)
    input_new = jnp.dot(new_normed, w_igate, preferred_element_type=jnp.float32)
    forget_new = jax.nn.log_sigmoid(jnp.dot(new_normed, w_fgate, preferred_element_type=jnp.float32) + forget_bias)
    top_next = jnp.maximum(forget_new + cache_top, input_new)
    old_share = jnp.exp(forget_new + cache_top - top_next)
    new_share = jnp.exp(input_new - top_next)
    agreement = lax.optimization_barrier(jnp.sum(key_new * query_new, axis=-1))
    factor = DH ** (-0.5)
    numerator = old_share[..., None] * jnp.einsum('shed,shd->she', cache_matrix.astype(jnp.float32), query_new)
    numerator = (numerator + (new_share * agreement)[..., None] * value_new) * factor
    denominator = (old_share * lax.optimization_barrier(jnp.sum(cache_normal * query_new, axis=-1)) + new_share * agreement) * factor
    read = numerator / jnp.maximum(jnp.abs(denominator), 1.0)[..., None]
    return (cache_matrix, cache_normal, cache_top, read.astype(jnp.bfloat16))
```

```python
import functools

import jax
import jax.numpy as jnp
from jax import lax
from jax.experimental import pallas as pl
from jax.experimental.pallas import tpu as pltpu
from jax.sharding import PartitionSpec as P

DH = 128
EPS = 1e-06
ROWS = 8
F32, BF16 = jnp.float32, jnp.bfloat16


def log1p_unit(u):
    z = u / (2.0 + u)
    q = z * z
    tail = jnp.full_like(q, 1.0 / 17)
    for odd in (15, 13, 11, 9, 7, 5, 3, 1):
        tail = tail * q + 1.0 / odd
    return 2.0 * z * tail


def log_sigmoid(x):
    return jnp.minimum(x, 0.0) - log1p_unit(jnp.exp(-jnp.abs(x)))


def normalize(rows):
    scaled = rows.astype(F32)
    mean = jnp.mean(scaled * scaled, axis=-1, keepdims=True)
    return (scaled * lax.rsqrt(mean + EPS)).astype(BF16)


def kernel(
    n, t, x_hbm, wk_hbm, wv_hbm, wq_hbm, wi_hbm, wf_hbm, bias_ref, new_hbm,
    mat_out, normal_out, top_out, read_out,
    x, wk, wv, wq, wi, wf, gw, gates, gates_new, keys, values, new_src, new_all, new_x,
    token, send, recv, stat_send, stat_recv,
    load_sem, new_send, new_recv, mat_send_sem, mat_recv_sem, stat_send_sem, stat_recv_sem,
):
    me, tp = lax.axis_index("sp"), lax.axis_index("tp")
    seqs, span, width = x.shape
    columns = wk.shape[1]
    heads = columns // DH
    all_heads = wi.shape[1]
    own = DH // n
    head_start = tp * heads
    up = lax.rem(2 * all_heads - head_start, 2 * all_heads)

    barrier = pltpu.get_barrier_semaphore()
    for k in range(1, n):
        pl.semaphore_signal(
            barrier, inc=1, device_id=(lax.rem(me + k, n), tp),
            device_id_type=pl.DeviceIdType.MESH)
    for k in range(1, t):
        pl.semaphore_signal(
            barrier, inc=1, device_id=(me, lax.rem(tp + k, t)),
            device_id_type=pl.DeviceIdType.MESH)

    pairs = [(new_hbm, new_src), (wi_hbm, wi), (wf_hbm, wf), (x_hbm.at[0], x.at[0]),
             (wk_hbm, wk), (wv_hbm, wv)]
    pairs += [(x_hbm.at[s], x.at[s]) for s in range(1, seqs)]
    pairs += [(wq_hbm, wq)]
    loads = [pltpu.make_async_copy(a, b, load_sem.at[i]) for i, (a, b) in enumerate(pairs)]
    for load in loads:
        load.start()
    new_load, wi_load, wf_load = loads[:3]
    x_loads = [loads[3]] + loads[6:6 + seqs - 1]
    wk_load, wv_load, wq_load = loads[4], loads[5], loads[-1]

    later = lax.broadcasted_iota(jnp.int32, (span, span), 0)
    earlier = lax.broadcasted_iota(jnp.int32, (span, span), 1)
    strict = (later > earlier).astype(F32).astype(BF16)
    head_row = lax.broadcasted_iota(jnp.int32, (ROWS, 1), 0)
    bias = jnp.zeros((ROWS, 1), F32)
    for h in range(heads):
        bias = jnp.where(head_row == h, bias_ref[head_start + h], bias)

    wi_load.wait()
    wf_load.wait()
    gw[...] = jnp.concatenate(
        [wi[...], wf[...], jnp.zeros((width, DH - 2 * all_heads), BF16)], axis=1)

    new_load.wait()
    pl.semaphore_wait(barrier, n - 1 + t - 1)
    new_copies = []
    for k in range(1, t):
        copy = pltpu.make_async_remote_copy(
            src_ref=new_src, dst_ref=new_all.at[tp],
            send_sem=new_send.at[k - 1], recv_sem=new_recv.at[k - 1],
            device_id=(me, lax.rem(tp + k, t)), device_id_type=pl.DeviceIdType.MESH)
        copy.start()
        new_copies.append(copy)
    new_all[tp] = new_src[...]

    block = 32 if span % 32 == 0 else span
    wide = 256 if columns % 256 == 0 else columns
    copies = []
    for s in range(seqs):
        x_loads[s].wait()

        def norm_step(i, carry):
            rows = pl.ds(pl.multiple_of(i * block, block), block)
            x[s, rows, :] = normalize(x[s, rows, :])
            return carry

        lax.fori_loop(0, span // block, norm_step, 0)

        gates[...] = jnp.dot(x[s], gw[...], preferred_element_type=F32).T
        own_gates = pltpu.roll(gates[:2 * all_heads, :], up, 0)
        igate = own_gates[:ROWS]
        logf = log_sigmoid(own_gates[all_heads:all_heads + ROWS] + bias)
        high = logf.astype(BF16).astype(F32)
        middle = (logf - high).astype(BF16).astype(F32)
        low = logf - high - middle
        parts = jnp.concatenate([high, middle, low, jnp.zeros_like(low)], axis=0).astype(BF16)
        sums = jnp.dot(parts, strict, preferred_element_type=F32)
        suffix = sums[:ROWS] + sums[ROWS:2 * ROWS] + sums[2 * ROWS:3 * ROWS]
        total = suffix[:, :1] + logf[:, :1]
        log_weight = suffix + igate
        top = jnp.max(log_weight, axis=1, keepdims=True)
        weight = jnp.exp(log_weight - top).T

        if s == 0:
            wk_load.wait()
            wv_load.wait()

        def project(c, carry):
            cols = pl.ds(pl.multiple_of(c * wide, wide), wide)
            keys[:, cols] = jnp.dot(x[s], wk[:, cols], preferred_element_type=F32).astype(BF16)
            values[:, cols] = jnp.dot(x[s], wv[:, cols], preferred_element_type=F32).astype(BF16)
            return carry

        lax.fori_loop(0, columns // wide, project, 0)

        lane = lax.broadcasted_iota(jnp.int32, (ROWS, DH), 1)
        stat_send[s, :ROWS, :] = jnp.zeros((ROWS, DH), F32)
        stat_send[s, ROWS:, :] = jnp.where(lane < DH // 2, top, total)
        for h in range(heads):
            share = weight[:, h:h + 1]
            key = keys[:, h * DH:(h + 1) * DH]
            value = values[:, h * DH:(h + 1) * DH]
            stat_send[s, h:h + 1, :] = jnp.sum(share * key.astype(F32), axis=0, keepdims=True)
            weighted = (share * value.astype(F32)).astype(BF16)
            part = lax.dot_general(
                weighted, key, (((0,), (0,)), ((), ())), preferred_element_type=F32)
            for j in range(n):
                send[s, j, h * own:(h + 1) * own, :] = part[j * own:(j + 1) * own].astype(send.dtype)
        for k in range(1, n):
            target = lax.rem(me + k, n)
            slot = s * (n - 1) + k - 1
            stat_copy = pltpu.make_async_remote_copy(
                src_ref=stat_send.at[s], dst_ref=stat_recv.at[s, me],
                send_sem=stat_send_sem.at[slot], recv_sem=stat_recv_sem.at[slot],
                device_id=(target, tp), device_id_type=pl.DeviceIdType.MESH)
            mat_copy = pltpu.make_async_remote_copy(
                src_ref=send.at[s, target], dst_ref=recv.at[s, me],
                send_sem=mat_send_sem.at[slot], recv_sem=mat_recv_sem.at[slot],
                device_id=(target, tp), device_id_type=pl.DeviceIdType.MESH)
            stat_copy.start()
            mat_copy.start()
            copies.append((s, stat_copy, mat_copy))
        stat_recv[s, me] = stat_send[s]
        recv[s, me] = send[s, me]

    for copy in new_copies:
        copy.wait()
    fresh = jnp.concatenate([new_all[i] for i in range(t)], axis=1)
    new_x[...] = jnp.zeros_like(new_x)
    new_x[:seqs, :] = normalize(fresh)
    rows = new_x[...]
    fresh_gates = jnp.dot(rows, gw[...], preferred_element_type=F32)
    gates_new[...] = jnp.concatenate(
        [fresh_gates, jnp.zeros((DH - 16, DH), F32)], axis=0).T
    wq_load.wait()
    token[...] = jnp.zeros_like(token)
    for which, w in enumerate((wq, wk, wv)):
        made = jnp.dot(rows, w[...], preferred_element_type=F32).astype(BF16).astype(F32)
        for s in range(seqs):
            for h in range(heads):
                token[which, s, h:h + 1, :] = made[s:s + 1, h * DH:(h + 1) * DH]
    own_new = pltpu.roll(gates_new[:2 * all_heads, :], up, 0)
    factor = DH ** (-0.5)
    turn = lax.rem(DH - me * own, DH)
    for s in range(seqs):
        query, key, value = token[0, s], token[1, s], token[2, s]
        igate_new = own_new[:ROWS, s:s + 1]
        logf_new = log_sigmoid(own_new[all_heads:all_heads + ROWS, s:s + 1] + bias)
        agreement = jnp.sum(key * query, axis=1, keepdims=True)
        value_own = pltpu.roll(value, turn, 1)[:, :own]

        for at, stat_copy, mat_copy in copies:
            if at == s:
                stat_copy.wait()
        beyond = jnp.zeros((ROWS, 1), F32)
        tops = [None] * n
        for j in reversed(range(n)):
            stat = stat_recv[s, j, ROWS:, :]
            tops[j] = beyond + stat[:, :1]
            beyond = beyond + stat[:, DH // 2:DH // 2 + 1]
        stabilizer = functools.reduce(jnp.maximum, tops)
        scales = [jnp.exp(top - stabilizer) for top in tops]
        normal = jnp.zeros((ROWS, DH), F32)
        for j in range(n):
            normal = normal + scales[j] * stat_recv[s, j, :ROWS, :]
        top_out[s] = jnp.broadcast_to(stabilizer, (ROWS, DH))
        normal_out[s] = pltpu.roll(normal, turn, 1)[:heads, :own]
        top_next = jnp.maximum(logf_new + stabilizer, igate_new)
        old_share = jnp.exp(logf_new + stabilizer - top_next)
        new_share = jnp.exp(igate_new - top_next)
        normal_dot = jnp.sum(normal * query, axis=1, keepdims=True)
        denominator = (old_share * normal_dot + new_share * agreement) * factor

        for at, stat_copy, mat_copy in copies:
            if at == s:
                mat_copy.wait()
        reading = jnp.zeros((ROWS, own), F32)
        query_low = query.astype(BF16)
        for h in range(heads):
            total = jnp.zeros((own, DH), F32)
            for j in range(n):
                piece = recv[s, j, h * own:(h + 1) * own, :].astype(F32)
                total = total + scales[j][h:h + 1, :] * piece
            stored = total.astype(BF16)
            mat_out[s, h] = stored
            seen = lax.dot_general(
                query_low, stored, (((1,), (1,)), ((), ())), preferred_element_type=F32)
            reading = jnp.where(head_row == h, seen, reading)
        numerator = (old_share * reading + (new_share * agreement) * value_own) * factor
        read = numerator / jnp.maximum(jnp.abs(denominator), 1.0)
        read_out[s] = read[:heads].astype(BF16)


def shards(n, t, inputs, w_key, w_value, w_query, w_igate, w_fgate, forget_bias, new_rows):
    seqs, span, width = inputs.shape
    columns = w_key.shape[1]
    heads = columns // DH
    own = DH // n
    all_heads = w_igate.shape[1]
    wire = BF16 if own % 16 == 0 else F32
    hbm = pl.BlockSpec(memory_space=pl.ANY)
    vmem = pl.BlockSpec(memory_space=pltpu.VMEM)
    scratch = [
        pltpu.VMEM((seqs, span, width), BF16),
        pltpu.VMEM((width, columns), BF16),
        pltpu.VMEM((width, columns), BF16),
        pltpu.VMEM((width, columns), BF16),
        pltpu.VMEM((width, all_heads), BF16),
        pltpu.VMEM((width, all_heads), BF16),
        pltpu.VMEM((width, DH), BF16),
        pltpu.VMEM((DH, span), F32),
        pltpu.VMEM((DH, DH), F32),
        pltpu.VMEM((span, columns), BF16),
        pltpu.VMEM((span, columns), BF16),
        pltpu.VMEM(new_rows.shape, BF16),
        pltpu.VMEM((t,) + new_rows.shape, BF16),
        pltpu.VMEM((16, width), BF16),
        pltpu.VMEM((3, seqs, ROWS, DH), F32),
        pltpu.VMEM((seqs, n, heads * own, DH), wire),
        pltpu.VMEM((seqs, n, heads * own, DH), wire),
        pltpu.VMEM((seqs, 2 * ROWS, DH), F32),
        pltpu.VMEM((seqs, n, 2 * ROWS, DH), F32),
        pltpu.SemaphoreType.DMA((7 + seqs - 1,)),
        pltpu.SemaphoreType.DMA((t - 1,)),
        pltpu.SemaphoreType.DMA((t - 1,)),
        pltpu.SemaphoreType.DMA((seqs * (n - 1),)),
        pltpu.SemaphoreType.DMA((seqs * (n - 1),)),
        pltpu.SemaphoreType.DMA((seqs * (n - 1),)),
        pltpu.SemaphoreType.DMA((seqs * (n - 1),)),
    ]
    matrix, normal, top, read = pl.pallas_call(
        functools.partial(kernel, n, t),
        out_shape=(
            jax.ShapeDtypeStruct((seqs, heads, own, DH), BF16),
            jax.ShapeDtypeStruct((seqs, heads, own), F32),
            jax.ShapeDtypeStruct((seqs, ROWS, DH), F32),
            jax.ShapeDtypeStruct((seqs, heads, own), BF16),
        ),
        in_specs=[hbm] * 6 + [pl.BlockSpec(memory_space=pltpu.SMEM), hbm],
        out_specs=(vmem,) * 4,
        scratch_shapes=scratch,
        compiler_params=pltpu.CompilerParams(
            collective_id=0, has_side_effects=True, vmem_limit_bytes=60 * 1024 * 1024),
    )(inputs, w_key, w_value, w_query, w_igate, w_fgate, forget_bias, new_rows)
    return matrix, normal, top[:, :heads, 0], read


def solution(mesh):
    in_specs = (
        P(None, "sp", None),
        P(None, "tp"),
        P(None, "tp"),
        P(None, "tp"),
        P(),
        P(),
        P(),
        P(None, "tp"),
    )
    out_specs = (P(None, "tp", "sp", None), P(None, "tp", "sp"), P(None, "tp"), P(None, "tp", "sp"))
    body = functools.partial(shards, mesh.shape["sp"], mesh.shape["tp"])
    return jax.shard_map(body, mesh=mesh, in_specs=in_specs, out_specs=out_specs, check_vma=False)
```

```python
import functools

import jax
import jax.numpy as jnp
from jax import lax
from jax.experimental import pallas as pl
from jax.experimental.pallas import tpu as pltpu
from jax.sharding import PartitionSpec as P

DH = 128
EPS = 1e-06
ROWS = 8
F32, BF16 = jnp.float32, jnp.bfloat16


def log1p_unit(u):
    z = u / (2.0 + u)
    q = z * z
    tail = jnp.full_like(q, 1.0 / 17)
    for odd in (15, 13, 11, 9, 7, 5, 3, 1):
        tail = tail * q + 1.0 / odd
    return 2.0 * z * tail


def log_sigmoid(x):
    return jnp.minimum(x, 0.0) - log1p_unit(jnp.exp(-jnp.abs(x)))


def normalize(rows):
    scaled = rows.astype(F32)
    mean = jnp.mean(scaled * scaled, axis=-1, keepdims=True)
    return (scaled * lax.rsqrt(mean + EPS)).astype(BF16)


def kernel(
    n, t, x_hbm, wk_hbm, wv_hbm, wq_hbm, wi_hbm, wf_hbm, bias_ref, new_hbm,
    mat_out, normal_out, top_out, read_out,
    x, wk, wv, wq, gw_rows, gw, gates_new, new_src, new_all, new_x,
    strict, token, send, recv, normal_send, normal_recv,
    load_sem, new_send, new_recv, mat_send_sem, mat_recv_sem,
    normal_send_sem, normal_recv_sem,
):
    me, tp = lax.axis_index("sp"), lax.axis_index("tp")
    seqs, span, width = x.shape
    columns = wk.shape[1]
    heads = columns // DH
    all_heads = wi_hbm.shape[0]
    own = DH // n
    head_start = tp * heads
    up = lax.rem(2 * all_heads - head_start, 2 * all_heads)
    wide = 256 if columns % 256 == 0 else columns
    chunks = columns // wide
    chunk_heads = wide // DH
    peers = [lax.rem(me + k, n) for k in range(1, n)]

    barrier = pltpu.get_barrier_semaphore()
    for peer in peers:
        pl.semaphore_signal(
            barrier, inc=1, device_id=(peer, tp), device_id_type=pl.DeviceIdType.MESH)
    for k in range(1, t):
        pl.semaphore_signal(
            barrier, inc=1, device_id=(me, lax.rem(tp + k, t)),
            device_id_type=pl.DeviceIdType.MESH)

    piece = 128 if span % 128 == 0 else span
    pieces = span // piece
    pairs = [(new_hbm, new_src), (wi_hbm, gw_rows.at[pl.ds(0, all_heads)]),
             (wf_hbm, gw_rows.at[pl.ds(all_heads, all_heads)])]
    pairs += [(x_hbm.at[0, pl.ds(i * piece, piece)], x.at[0, pl.ds(i * piece, piece)])
              for i in range(pieces)]
    pairs += [(wk_hbm, wk), (wv_hbm, wv)]
    pairs += [(x_hbm.at[s], x.at[s]) for s in range(1, seqs)]
    pairs += [(wq_hbm, wq)]
    loads = [pltpu.make_async_copy(a, b, load_sem.at[i]) for i, (a, b) in enumerate(pairs)]
    for load in loads:
        load.start()
    new_load, wi_load, wf_load = loads[:3]
    first_loads = loads[3:3 + pieces]
    wk_load, wv_load = loads[3 + pieces:5 + pieces]
    x_loads = [None] + loads[5 + pieces:-1]
    wq_load = loads[-1]

    later = lax.broadcasted_iota(jnp.int32, (span, span), 0)
    earlier = lax.broadcasted_iota(jnp.int32, (span, span), 1)
    strict[...] = (later > earlier).astype(F32).astype(BF16)
    head_row = lax.broadcasted_iota(jnp.int32, (ROWS, 1), 0)
    lane = lax.broadcasted_iota(jnp.int32, (ROWS, DH), 1)
    bias = jnp.zeros((ROWS, 1), F32)
    for h in range(heads):
        bias = jnp.where(head_row == h, bias_ref[head_start + h], bias)

    block = 16 if span % 16 == 0 else span

    def norm_rows(s, start, stop):
        for at in range(start, stop, block):
            x[s, at:at + block, :] = normalize(x[s, at:at + block, :])

    def push(src, dst, send_sem, recv_sem, peer):
        copy = pltpu.make_async_remote_copy(
            src_ref=src, dst_ref=dst, send_sem=send_sem, recv_sem=recv_sem,
            device_id=(peer, tp), device_id_type=pl.DeviceIdType.MESH)
        copy.start()
        return copy

    wi_load.wait()
    wf_load.wait()
    gw[...] = jnp.concatenate(
        [gw_rows[...], jnp.zeros((DH - 2 * all_heads, width), BF16)], axis=0).T
    for i in range(pieces):
        first_loads[i].wait()
        norm_rows(0, i * piece, (i + 1) * piece)

    normal_copies, mat_copies, new_copies = {}, {}, []
    for s in range(seqs):
        if s == 0:
            wk_load.wait()
        gates = jnp.dot(x[s], gw[...], preferred_element_type=F32).T
        own_gates = pltpu.roll(gates[:2 * all_heads, :], up, 0)
        igate = own_gates[:ROWS]
        logf = log_sigmoid(own_gates[all_heads:all_heads + ROWS] + bias)
        high = logf.astype(BF16).astype(F32)
        middle = (logf - high).astype(BF16).astype(F32)
        low = logf - high - middle
        parts = jnp.concatenate([high, middle, low, jnp.zeros_like(low)], axis=0).astype(BF16)
        sums = jnp.dot(parts, strict[...], preferred_element_type=F32)
        suffix = sums[:ROWS] + sums[ROWS:2 * ROWS] + sums[2 * ROWS:3 * ROWS]
        total = suffix[:, :1] + logf[:, :1]
        log_weight = suffix + igate
        top = jnp.max(log_weight, axis=1, keepdims=True)
        weight = jnp.exp(log_weight - top)
        high = weight.astype(BF16).astype(F32)
        middle = (weight - high).astype(BF16).astype(F32)
        weights = jnp.concatenate(
            [high, middle, weight - high - middle, jnp.zeros_like(high)], axis=0).astype(BF16)
        stat = jnp.where(lane < DH // 2, top, total)
        normal_send[s, :ROWS, :] = jnp.zeros((ROWS, DH), F32)
        normal_send[s, ROWS:, :] = stat

        for c in range(chunks):
            cols = slice(c * wide, (c + 1) * wide)
            last = c == chunks - 1
            keys = jnp.dot(x[s], wk[:, cols], preferred_element_type=F32).astype(BF16)
            if s == 0 and c == 0:
                wv_load.wait()
                new_load.wait()
                pl.semaphore_wait(barrier, n - 1 + t - 1)
                for k in range(1, t):
                    copy = pltpu.make_async_remote_copy(
                        src_ref=new_src, dst_ref=new_all.at[tp],
                        send_sem=new_send.at[k - 1], recv_sem=new_recv.at[k - 1],
                        device_id=(me, lax.rem(tp + k, t)),
                        device_id_type=pl.DeviceIdType.MESH)
                    copy.start()
                    new_copies.append(copy)
                new_all[tp] = new_src[...]
            if last and s + 1 < seqs:
                x_loads[s + 1].wait()
                norm_rows(s + 1, 0, span)
            values = jnp.dot(x[s], wv[:, cols], preferred_element_type=F32).astype(BF16)
            sums = jnp.dot(weights, keys, preferred_element_type=F32)
            sums = sums[:ROWS] + sums[ROWS:2 * ROWS] + sums[2 * ROWS:3 * ROWS]
            flipped = values.T
            for i in range(chunk_heads):
                h = c * chunk_heads + i
                normal_send[s, h:h + 1, :] = sums[h:h + 1, i * DH:(i + 1) * DH]
                value = flipped[i * DH:(i + 1) * DH].astype(F32)
                weighted = (weight[h:h + 1, :] * value).astype(BF16)
                part = jnp.dot(
                    weighted, keys[:, i * DH:(i + 1) * DH], preferred_element_type=F32)
                for j in range(n):
                    send[s, j, c, i * own:(i + 1) * own, :] = (
                        part[j * own:(j + 1) * own].astype(send.dtype))
        normal_copies[s] = [
            push(normal_send.at[s], normal_recv.at[s, me],
                 normal_send_sem.at[s * (n - 1) + k], normal_recv_sem.at[s * (n - 1) + k],
                 peer) for k, peer in enumerate(peers)]
        normal_recv[s, me] = normal_send[s]
        mat_copies[s] = [
            push(send.at[s, peer], recv.at[s, me],
                 mat_send_sem.at[s * (n - 1) + k], mat_recv_sem.at[s * (n - 1) + k], peer)
            for k, peer in enumerate(peers)]
        recv[s, me] = send[s, me]

    for copy in new_copies:
        copy.wait()
    fresh = jnp.concatenate([new_all[i] for i in range(t)], axis=1)
    new_x[...] = jnp.zeros_like(new_x)
    new_x[:seqs, :] = normalize(fresh)
    rows = new_x[...]
    fresh_gates = jnp.dot(rows, gw[...], preferred_element_type=F32)
    gates_new[...] = jnp.concatenate(
        [fresh_gates, jnp.zeros((DH - 16, DH), F32)], axis=0).T
    wq_load.wait()
    token[...] = jnp.zeros_like(token)
    for which, w in enumerate((wq, wk, wv)):
        made = jnp.dot(rows, w[...], preferred_element_type=F32).astype(BF16).astype(F32)
        for s in range(seqs):
            for h in range(heads):
                token[which, s, h:h + 1, :] = made[s:s + 1, h * DH:(h + 1) * DH]
    own_new = pltpu.roll(gates_new[:2 * all_heads, :], up, 0)
    factor = DH ** (-0.5)
    turn = lax.rem(DH - me * own, DH)
    for s in range(seqs):
        query, key, value = token[0, s], token[1, s], token[2, s]
        igate_new = own_new[:ROWS, s:s + 1]
        logf_new = log_sigmoid(own_new[all_heads:all_heads + ROWS, s:s + 1] + bias)
        agreement = jnp.sum(key * query, axis=1, keepdims=True)
        value_own = pltpu.roll(value, turn, 1)[:, :own]

        for copy in normal_copies[s]:
            copy.wait()
        beyond = jnp.zeros((ROWS, 1), F32)
        tops = [None] * n
        for j in reversed(range(n)):
            stat = normal_recv[s, j, ROWS:, :]
            tops[j] = beyond + stat[:, :1]
            beyond = beyond + stat[:, DH // 2:DH // 2 + 1]
        stabilizer = functools.reduce(jnp.maximum, tops)
        scales = [jnp.exp(top - stabilizer) for top in tops]
        top_row = jnp.sum(jnp.where(lane == head_row, stabilizer, 0.0), axis=0, keepdims=True)
        top_out[s:s + 1, :] = top_row[:, :heads]
        top_next = jnp.maximum(logf_new + stabilizer, igate_new)
        old_share = jnp.exp(logf_new + stabilizer - top_next)
        new_share = jnp.exp(igate_new - top_next)
        reading = jnp.zeros((ROWS, own), F32)
        query_low = query.astype(BF16)
        for c in range(chunks):
            for copy in mat_copies[s] if c == 0 else ():
                copy.wait()
            for i in range(chunk_heads):
                h = c * chunk_heads + i
                total = jnp.zeros((own, DH), F32)
                for j in range(n):
                    part = recv[s, j, c, i * own:(i + 1) * own, :].astype(F32)
                    total = total + scales[j][h:h + 1, :] * part
                stored = total.astype(BF16)
                mat_out[s, h] = stored
                seen = lax.dot_general(
                    query_low, stored, (((1,), (1,)), ((), ())), preferred_element_type=F32)
                reading = jnp.where(head_row == h, seen, reading)
        normal = jnp.zeros((ROWS, DH), F32)
        for j in range(n):
            normal = normal + scales[j] * normal_recv[s, j, :ROWS, :]
        normal_out[s] = pltpu.roll(normal, turn, 1)[:heads, :own]
        normal_dot = jnp.sum(normal * query, axis=1, keepdims=True)
        denominator = (old_share * normal_dot + new_share * agreement) * factor
        numerator = (old_share * reading + (new_share * agreement) * value_own) * factor
        read = numerator / jnp.maximum(jnp.abs(denominator), 1.0)
        read_out[s] = read[:heads].astype(BF16)


def hand_on(*refs):
    count = (len(refs) - 2) // 3
    sources, targets, held = (refs[i * count:(i + 1) * count] for i in range(3))
    come, go = refs[-2:]
    ins = [pltpu.make_async_copy(a, b, come.at[i])
           for i, (a, b) in enumerate(zip(sources, held))]
    outs = [pltpu.make_async_copy(a, b, go.at[i])
            for i, (a, b) in enumerate(zip(held, targets))]
    for copy in ins:
        copy.start()
    for copy, on in zip(ins, outs):
        copy.wait()
        on.start()
    for on in outs:
        on.wait()


def shards(n, t, inputs, w_key, w_value, w_query, w_igate, w_fgate, forget_bias, new_rows):
    seqs, span, width = inputs.shape
    columns = w_key.shape[1]
    heads = columns // DH
    own = DH // n
    all_heads = w_igate.shape[1]
    wire = BF16 if own % 16 == 0 else F32
    hbm = pl.BlockSpec(memory_space=pl.ANY)
    vmem = pl.BlockSpec(memory_space=pltpu.VMEM)
    wide = 256 if columns % 256 == 0 else columns
    chunks = columns // wide
    slab = pltpu.VMEM((seqs, n, chunks, wide // DH * own, DH), wire)
    small = [pltpu.SemaphoreType.DMA((seqs * (n - 1),))] * 2
    scratch = [
        pltpu.VMEM((seqs, span, width), BF16),
        pltpu.VMEM((width, columns), BF16),
        pltpu.VMEM((width, columns), BF16),
        pltpu.VMEM((width, columns), BF16),
        pltpu.VMEM((2 * all_heads, width), BF16),
        pltpu.VMEM((width, DH), BF16),
        pltpu.VMEM((DH, DH), F32),
        pltpu.VMEM(new_rows.shape, BF16),
        pltpu.VMEM((t,) + new_rows.shape, BF16),
        pltpu.VMEM((16, width), BF16),
        pltpu.VMEM((span, span), BF16),
        pltpu.VMEM((3, seqs, ROWS, DH), F32),
        slab,
        slab,
        pltpu.VMEM((seqs, 2 * ROWS, DH), F32),
        pltpu.VMEM((seqs, n, 2 * ROWS, DH), F32),
        pltpu.SemaphoreType.DMA((5 + max(1, span // 128) + seqs,)),
        pltpu.SemaphoreType.DMA((t - 1,)),
        pltpu.SemaphoreType.DMA((t - 1,)),
        pltpu.SemaphoreType.DMA((seqs * (n - 1),)),
        pltpu.SemaphoreType.DMA((seqs * (n - 1),)),
    ] + small
    out_shape = (
        jax.ShapeDtypeStruct((seqs, heads, own, DH), BF16),
        jax.ShapeDtypeStruct((seqs, heads, own), F32),
        jax.ShapeDtypeStruct((seqs, heads), F32),
        jax.ShapeDtypeStruct((seqs, heads, own), BF16),
    )
    made = pl.pallas_call(
        functools.partial(kernel, n, t),
        out_shape=out_shape,
        in_specs=[hbm] * 6 + [pl.BlockSpec(memory_space=pltpu.SMEM), hbm],
        out_specs=(vmem,) * 4,
        scratch_shapes=scratch,
        compiler_params=pltpu.CompilerParams(
            collective_id=0, has_side_effects=True, vmem_limit_bytes=60 * 1024 * 1024),
    )(inputs, w_key, w_value, w_query, w_igate.T, w_fgate.T, forget_bias, new_rows)
    return pl.pallas_call(
        hand_on, out_shape=out_shape, in_specs=[hbm] * 4, out_specs=(hbm,) * 4,
        scratch_shapes=[pltpu.VMEM(out.shape, out.dtype) for out in out_shape]
        + [pltpu.SemaphoreType.DMA((4,))] * 2,
        compiler_params=pltpu.CompilerParams(vmem_limit_bytes=60 * 1024 * 1024),
    )(*made)


def solution(mesh):
    in_specs = (
        P(None, "sp", None),
        P(None, "tp"),
        P(None, "tp"),
        P(None, "tp"),
        P(),
        P(),
        P(),
        P(None, "tp"),
    )
    out_specs = (P(None, "tp", "sp", None), P(None, "tp", "sp"), P(None, "tp"), P(None, "tp", "sp"))
    body = functools.partial(shards, mesh.shape["sp"], mesh.shape["tp"])
    return jax.shard_map(body, mesh=mesh, in_specs=in_specs, out_specs=out_specs, check_vma=False)
```
